512 devices in a mesh: kv: 64 (over z, y), tp: 8 (over x, core).
Axes of the slice: x: 4, y: 8, z: 8, core: 2. Of those that a mesh axis runs over, the one named last changes fastest.
Arguments:
- hidden_in: bfloat16 [1024, 2048], P('kv', 'tp'), may hold values from -6 to 6
- first_gain: bfloat16 [2048], P('tp'), may hold values from 0.099609375 to 1.8984375
- first_gate_proj: bfloat16 [2048, 5632], P('tp', 'kv'), may hold values from -0.125 to 0.125
- first_up_proj: bfloat16 [2048, 5632], P('tp', 'kv'), may hold values from -0.125 to 0.125
- first_down_proj: bfloat16 [5632, 2048], P('kv', 'tp'), may hold values from -0.078125 to 0.078125
- mix_gain: bfloat16 [2048], replicated, may hold values from 0.099609375 to 1.8984375
- query_weight: bfloat16 [2048, 1024], P(None, 'tp'), may hold values from -0.125 to 0.125
- forget_weight: bfloat16 [2048, 1024], P(None, 'tp'), may hold values from -0.125 to 0.125
- input_weight: bfloat16 [2048, 1024], P(None, 'tp'), may hold values from -0.125 to 0.125
- outgate_weight: bfloat16 [2048, 1024], P(None, 'tp'), may hold values from -0.125 to 0.125
- forget_floor: float32 [1024], P('tp'), may hold values from 0.05 to 0.95
- state_in: float32 [1024, 8, 128, 128], P('kv', 'tp'), may hold values from -6 to 6
- out_gain: bfloat16 [1024], P('tp'), may hold values from 0.099609375 to 1.8984375
- mix_out_weight: bfloat16 [1024, 2048], P('tp'), may hold values from -0.1875 to 0.1875
- second_gain: bfloat16 [2048], P('tp'), may hold values from 0.099609375 to 1.8984375
- second_gate_proj: bfloat16 [2048, 5632], P('tp', 'kv'), may hold values from -0.125 to 0.125
- second_up_proj: bfloat16 [2048, 5632], P('tp', 'kv'), may hold values from -0.125 to 0.125
- second_down_proj: bfloat16 [5632, 2048], P('kv', 'tp'), may hold values from -0.078125 to 0.078125
Outputs:
- hidden_out: bfloat16 [1024, 2048], P('kv', 'tp')
- state_out: float32 [1024, 8, 128, 128], P('kv', 'tp')
The draws below stay inside these ranges and needn't reach their ends.
All inputs are finite; a program needn't handle non-finite values.
Results may differ from the reference program's by a relative error of at most 0.019.
Values may be sent and summed in bfloat16 or wider, within the bound.
A program may use at most 64 MiB of HBM per device.

```python
import jax
import jax.numpy as jnp
from jax import lax

D = 2048
FF = 5632
HEADS = 8
HEAD = 128
BATCH = 1024
HK = 1024
N_TP = 8


def levels(stream_key, shape, pieces, low, high):
    def one(position, parts):
        draws = jax.random.uniform(jax.random.fold_in(jax.random.fold_in(stream_key, 6), position), (parts,), jnp.float32, low / len(pieces), high / len(pieces))
        return jnp.repeat(jnp.exp(draws), shape[position] // parts).reshape((-1,) + (1,) * (len(shape) - position - 1))

    loudness = one(*pieces[0])
    for cut in pieces[1:]:
        loudness = loudness * one(*cut)
    return loudness


def gaussian(key, shape, scale, most, pieces=(), dtype=jnp.bfloat16):
    level = levels(key, shape, pieces, -0.22, 0.18) if pieces else 1.0
    result = jax.random.normal(key, shape, jnp.float32) * scale * level
    return jnp.minimum(jnp.maximum(result, -most), most).astype(dtype)


def setup_inputs(seed: int = 0) -> dict:
    arg_keys = jax.random.split(jax.random.key(seed), 19)
    return {
        "hidden_in": gaussian(arg_keys[0], (BATCH, D), 1.0, 6.0, ((0, 64), (1, 8))),
        "first_gain": jnp.clip(1.0 + 0.18 * jax.random.normal(arg_keys[1], (D,), jnp.float32), 0.099609375, 1.8984375).astype(jnp.bfloat16),
        "first_gate_proj": gaussian(arg_keys[2], (D, FF), D ** -0.5, 0.125, ((0, 8), (1, 64))),
        "first_up_proj": gaussian(arg_keys[3], (D, FF), D ** -0.5, 0.125, ((0, 8), (1, 64))),
        "first_down_proj": gaussian(arg_keys[4], (FF, D), FF ** -0.5, 0.078125, ((0, 64), (1, 8))),
        "mix_gain": jnp.clip(1.0 + 0.18 * jax.random.normal(arg_keys[5], (D,), jnp.float32), 0.099609375, 1.8984375).astype(jnp.bfloat16),
        "query_weight": gaussian(arg_keys[6], (D, HK), D ** -0.5, 0.125, ((1, 8),)),
        "forget_weight": gaussian(arg_keys[7], (D, HK), D ** -0.5, 0.125, ((1, 8),)),
        "input_weight": gaussian(arg_keys[8], (D, HK), D ** -0.5, 0.125, ((1, 8),)),
        "outgate_weight": gaussian(arg_keys[9], (D, HK), D ** -0.5, 0.125, ((1, 8),)),
        "forget_floor": jnp.clip(0.05 + 0.9 * jax.random.uniform(arg_keys[10], (HK,), jnp.float32) ** levels(arg_keys[10], (HK,), ((0, 8),), -0.2, 0.2), 0.05, 0.95),
        "state_in": gaussian(arg_keys[11], (BATCH, HEADS, HEAD, HEAD), 1.0, 6.0, ((0, 64), (1, 8)), jnp.float32),
        "out_gain": jnp.clip(1.0 + 0.18 * jax.random.normal(arg_keys[12], (HK,), jnp.float32), 0.099609375, 1.8984375).astype(jnp.bfloat16),
        "mix_out_weight": gaussian(arg_keys[13], (HK, D), HK ** -0.5, 0.1875, ((0, 8),)),
        "second_gain": jnp.clip(1.0 + 0.18 * jax.random.normal(arg_keys[14], (D,), jnp.float32), 0.099609375, 1.8984375).astype(jnp.bfloat16),
        "second_gate_proj": gaussian(arg_keys[15], (D, FF), D ** -0.5, 0.125, ((0, 8), (1, 64))),
        "second_up_proj": gaussian(arg_keys[16], (D, FF), D ** -0.5, 0.125, ((0, 8), (1, 64))),
        "second_down_proj": gaussian(arg_keys[17], (FF, D), FF ** -0.5, 0.078125, ((0, 64), (1, 8))),
    }


def feed_forward(hidden, norm_gain, gate_proj, up_proj, down_proj):
    values = hidden.astype(jnp.float32)
    inverse = lax.rsqrt(lax.optimization_barrier(jnp.mean(values * values, axis=1, keepdims=True)) + 1e-06)
    scaled = (values * norm_gain.astype(jnp.float32)).astype(jnp.bfloat16)
    gate_sum = jnp.dot(scaled, gate_proj, preferred_element_type=jnp.float32) * inverse
    up_sum = jnp.dot(scaled, up_proj, preferred_element_type=jnp.float32) * inverse
    inner_units = (jax.nn.silu(gate_sum) * up_sum).astype(jnp.bfloat16)
    down_sum = jnp.dot(inner_units, down_proj, preferred_element_type=jnp.float32)
    return (values + 0.5 * down_sum).astype(jnp.bfloat16)

def reference(hidden_in, first_gain, first_gate_proj, first_up_proj, first_down_proj, mix_gain, query_weight, forget_weight, input_weight, outgate_weight, forget_floor, state_in, out_gain, mix_out_weight, second_gain, second_gate_proj, second_up_proj, second_down_proj):
    first_out = feed_forward(hidden_in, first_gain, first_gate_proj, first_up_proj, first_down_proj)
    values = first_out.astype(jnp.float32)
    inverse = lax.rsqrt(lax.optimization_barrier(jnp.mean(values * values, axis=1, keepdims=True)) + 1e-06)
    normed = (values * inverse * mix_gain.astype(jnp.float32)).astype(jnp.bfloat16)
    batch_size = hidden_in.shape[0]

    def project(weight):
        return jnp.dot(normed, weight, preferred_element_type=jnp.float32).reshape(batch_size, HEADS, HEAD)
    query_vals = jax.nn.silu(project(query_weight))
    forget_pre = project(forget_weight)
    input_vals = project(input_weight)
    out_gate = project(outgate_weight)
    floor_vals = forget_floor.reshape(HEADS, HEAD)
    log_forget = jnp.logaddexp(jnp.log(floor_vals), jnp.log1p(-floor_vals) + jax.nn.log_sigmoid(forget_pre))
    key_vals = -jnp.expm1(log_forget)
    new_state = jnp.exp(log_forget)[..., None] * state_in + key_vals[..., None] * input_vals[:, :, None, :]
    readout = jnp.einsum('bhk,bhkv->bhv', query_vals, new_state, precision=lax.Precision.HIGHEST)
    normed_out = readout * lax.rsqrt(lax.optimization_barrier(jnp.mean(readout * readout, axis=-1, keepdims=True)) + 1e-05) * out_gain.astype(jnp.float32).reshape(HEADS, HEAD)
    gated_out = (normed_out * jax.nn.silu(out_gate)).reshape(batch_size, HK).astype(jnp.bfloat16)
    group_width = HK // N_TP
    gated_groups = gated_out.reshape(batch_size, N_TP, group_width).astype(jnp.float32)
    weight_groups = mix_out_weight.reshape(N_TP, group_width, D).astype(jnp.float32)
    partial_value = jnp.einsum('bgk,gkd->bgd', gated_groups, weight_groups).astype(jnp.bfloat16)
    mixed_sum = lax.optimization_barrier(jnp.sum(partial_value.astype(jnp.float32), axis=1))
    second_in = (values + mixed_sum).astype(jnp.bfloat16)
    hidden_out = feed_forward(second_in, second_gain, second_gate_proj, second_up_proj, second_down_proj)
    return (hidden_out, new_state)
```

```python
import functools

import jax
import jax.numpy as jnp
from jax import lax
from jax.experimental import pallas as pl
from jax.experimental.pallas import tpu as pltpu
from jax.sharding import PartitionSpec as P

MESH = pl.DeviceIdType.MESH
F32 = jnp.float32
BF16 = jnp.bfloat16
ROWS = 16
WIDTH = 256
HALF = 128
HID = 88
HEAD = 128
GATE, UP, DOWN = 0, 1, 2
ROW_DIMS = (((1,), (1,)), ((), ()))


def kernel(
    n,
    hidden_hbm,
    params_hbm,
    gate1_hbm,
    up1_hbm,
    down1_hbm,
    gate2_hbm,
    up2_hbm,
    down2_hbm,
    query_hbm,
    forget_hbm,
    input_hbm,
    outgate_hbm,
    mixout_hbm,
    state_hbm,
    hidden_out_hbm,
    state_out_hbm,
    hid,
    par,
    gains,
    weights,
    wmix,
    wout,
    state,
    act,
    part,
    red0,
    red1,
    sum0,
    sum1,
    own0,
    own1,
    mid,
    rows_in,
    mix_send,
    mix_recv,
    last,
    load_sem,
    gain_send,
    gain_recv,
    w_send,
    w_recv,
    a_send,
    a_recv,
    b_send,
    b_recv,
    c_send,
    c_recv,
    d_send,
    d_recv,
    x_send,
    x_recv,
    m_send,
    m_recv,
):
    kv = lax.axis_index("kv")
    tp = lax.axis_index("tp")
    z, y = lax.div(kv, n), lax.rem(kv, n)
    group = lax.rem(z + y, n)
    src_y = lax.rem(tp - z + n, n)
    src_z = lax.rem(tp - y + n, n)
    home = tp == group
    pair = tp + 1 - 2 * lax.rem(tp, 2)
    far_first = sorted(range(1, n), key=lambda d: -min(d, n - d))

    def at(zz, yy, tt):
        return {"kv": zz * n + yy, "tp": tt}

    def up(index, d):
        return lax.rem(index + d, n)

    def rows_of(zz):
        return pl.ds(pl.multiple_of(zz * ROWS, ROWS), ROWS)

    loads = [
        pltpu.make_async_copy(hidden_hbm, hid, load_sem.at[0]),
        pltpu.make_async_copy(params_hbm, par, load_sem.at[1]),
        pltpu.make_async_copy(gate1_hbm, weights.at[0, tp, GATE], load_sem.at[2]),
        pltpu.make_async_copy(up1_hbm, weights.at[0, tp, UP], load_sem.at[3]),
        pltpu.make_async_copy(down1_hbm, weights.at[0, tp, DOWN], load_sem.at[4]),
        pltpu.make_async_copy(gate2_hbm, weights.at[1, tp, GATE], load_sem.at[5]),
        pltpu.make_async_copy(up2_hbm, weights.at[1, tp, UP], load_sem.at[6]),
        pltpu.make_async_copy(down2_hbm, weights.at[1, tp, DOWN], load_sem.at[7]),
        pltpu.make_async_copy(query_hbm, wmix.at[:, 0:HEAD], load_sem.at[8]),
        pltpu.make_async_copy(forget_hbm, wmix.at[:, HEAD : 2 * HEAD], load_sem.at[9]),
        pltpu.make_async_copy(input_hbm, wmix.at[:, 2 * HEAD : 3 * HEAD], load_sem.at[10]),
        pltpu.make_async_copy(outgate_hbm, wmix.at[:, 3 * HEAD :], load_sem.at[11]),
        pltpu.make_async_copy(mixout_hbm, wout, load_sem.at[12]),
        pltpu.make_async_copy(state_hbm, state, load_sem.at[13]),
    ]
    for load in loads:
        load.start()

    barrier = pltpu.get_barrier_semaphore()

    def greet(device):
        pl.semaphore_signal(barrier, inc=1, device_id=device, device_id_type=MESH)

    for d in range(1, n):
        greet(at(z, y, up(tp, d)))
        greet(at(up(z, d), y, tp))
        greet(at(z, up(y, d), tp))
        greet(at(z, up(y, d), group))
        greet(at(up(z, d), y, group))

    @pl.when(jnp.logical_not(home))
    def _():
        for d in range(n):
            greet(at(z, src_y, up(tp, d)))
            greet(at(src_z, y, up(tp, d)))

    for load in loads[:8]:
        load.wait()
    gains[tp] = par[8:16]

    pl.semaphore_wait(barrier, 5 * (n - 1) + jnp.where(home, 0, 2 * n))

    sends = []

    def send(src, dst, send_sem, recv_sem, device):
        copy = pltpu.make_async_remote_copy(
            src_ref=src,
            dst_ref=dst,
            send_sem=send_sem,
            recv_sem=recv_sem,
            device_id=device,
            device_id_type=MESH,
        )
        copy.start()
        sends.append((copy, None))

    def send_or_keep(here, src, dst, send_sem, recv_sem, device):
        away = pltpu.make_async_remote_copy(
            src_ref=src,
            dst_ref=dst,
            send_sem=send_sem,
            recv_sem=recv_sem,
            device_id=device,
            device_id_type=MESH,
        )

        @pl.when(here)
        def _():
            pltpu.make_async_copy(src, dst, recv_sem).start()

        @pl.when(jnp.logical_not(here))
        def _():
            away.start()

        sends.append((away, here))

    def arrived(dst, sem):
        pltpu.make_async_copy(dst, dst, sem).wait()

    def weights_of(kind, f, slot):
        return weights.at[f, slot, GATE:DOWN] if kind == 0 else weights.at[f, slot, DOWN]

    def send_weights(kind, f):
        for k in range(1, n // 2):
            send(
                weights_of(kind, f, tp),
                weights_of(kind, f, tp),
                w_send.at[kind, f, k],
                w_recv.at[kind, f, tp],
                at(z, y, up(tp, 2 * k)),
            )
        send(weights_of(kind, f, tp), weights_of(kind, f, tp), w_send.at[kind, f, 0], w_recv.at[kind, f, tp], at(z, y, pair))

    def pass_weights(kind, f):
        for k in range(1, n // 2):
            slot = up(tp, 2 * k)
            arrived(weights_of(kind, f, slot), w_recv.at[kind, f, slot])
            send(
                weights_of(kind, f, slot),
                weights_of(kind, f, slot),
                w_send.at[kind, f, n // 2 + k],
                w_recv.at[kind, f, slot],
                at(z, y, pair),
            )

    def take_weights(kind, f):
        for k in range(n // 2):
            slot = up(pair, 2 * k)
            arrived(weights_of(kind, f, slot), w_recv.at[kind, f, slot])

    def spread(f, block):
        for d in [0] + far_first:
            to_row = at(z, up(y, d), group)
            to_col = at(up(z, d), y, group)
            row_args = (
                block.at[:, 0:HALF],
                act.at[f, tp, rows_of(z), 0:HALF],
                a_send.at[f, 0, d],
                a_recv.at[f, 0, tp],
                to_row,
            )
            col_args = (
                block.at[:, HALF:WIDTH],
                act.at[f, tp, rows_of(z), HALF:WIDTH],
                a_send.at[f, 1, d],
                a_recv.at[f, 1, tp],
                to_col,
            )
            if d == 0:
                send_or_keep(home, *row_args)
                send_or_keep(home, *col_args)
            else:
                send(*row_args)
                send(*col_args)

    def gather(f):
        for t in range(n):
            arrived(act.at[f, t, rows_of(z), 0:HALF], a_recv.at[f, 0, t])
        region = act.at[f, :, rows_of(z), 0:HALF]
        for d in far_first:
            send(region, region, b_send.at[f, 0, d], b_recv.at[f, 0, d], at(up(z, d), y, tp))
        for t in range(n):
            arrived(act.at[f, t, rows_of(src_z), HALF:WIDTH], a_recv.at[f, 1, t])
        region = act.at[f, :, rows_of(src_z), HALF:WIDTH]
        for d in far_first:
            send(region, region, b_send.at[f, 1, d], b_recv.at[f, 1, d], at(z, up(y, d), tp))

    def gathered(f):
        for d in range(1, n):
            arrived(act.at[f, :, rows_of(up(z, n - d)), 0:HALF], b_recv.at[f, 0, d])
            arrived(
                act.at[f, :, rows_of(up(src_z, d)), HALF:WIDTH], b_recv.at[f, 1, d]
            )

    def inner_units(f):
        gate = jnp.zeros((n * ROWS, HID), F32)
        up_total = jnp.zeros((n * ROWS, HID), F32)
        squares = jnp.zeros((n * ROWS, HALF), F32)
        for t in range(n):
            values = act[f, t].astype(F32)
            squares += values[:, 0:HALF] * values[:, 0:HALF]
            squares += values[:, HALF:WIDTH] * values[:, HALF:WIDTH]
            scaled = (values * gains[t, f : f + 1, :]).astype(BF16)
            gate += lax.dot_general(scaled, weights[f, t, GATE], ROW_DIMS, preferred_element_type=F32)
            up_total += lax.dot_general(scaled, weights[f, t, UP], ROW_DIMS, preferred_element_type=F32)
        inverse = lax.rsqrt(jnp.sum(squares, axis=1, keepdims=True) / (n * WIDTH) + 1e-06)
        gate = gate * inverse
        return (gate * jax.nn.sigmoid(gate) * (up_total * inverse)).astype(BF16)

    def scatter(f, units):
        for t in range(n):
            part[f, t] = jnp.dot(
                units, weights[f, t, DOWN], preferred_element_type=F32
            ).astype(BF16)
        for d in far_first:
            to_z, to_y = up(z, d), up(y, d)
            send(
                part.at[f, :, rows_of(to_z), 0:HALF],
                red0.at[f, d],
                c_send.at[f, 0, d],
                c_recv.at[f, 0, d],
                at(to_z, y, tp),
            )
            send(
                part.at[f, :, rows_of(lax.rem(tp - to_y + n, n)), HALF:WIDTH],
                red1.at[f, d],
                c_send.at[f, 1, d],
                c_recv.at[f, 1, d],
                at(z, to_y, tp),
            )

    def reduce(f):
        for half, red, summed, lanes, row in (
            (0, red0, sum0, slice(0, HALF), z),
            (1, red1, sum1, slice(HALF, WIDTH), src_z),
        ):
            total = part[f, :, rows_of(row), lanes].astype(F32)
            for d in range(1, n):
                arrived(red.at[f, d], c_recv.at[f, half, d])
                total += red[f, d].astype(F32)
            summed[f] = total.astype(BF16)
            for e in [0] + far_first:
                tt = up(tp, e)
                if half == 0:
                    args = (sum0.at[f, tt], own0.at[f, y], d_send.at[f, 0, e], d_recv.at[f, 0, y])
                    device = at(z, src_y, tt)
                else:
                    args = (sum1.at[f, tt], own1.at[f, z], d_send.at[f, 1, e], d_recv.at[f, 1, z])
                    device = at(src_z, y, tt)
                if e == 0:
                    send_or_keep(home, *args, device)
                else:
                    send(*args, device)

    def reduced(f):
        for k in range(n):
            arrived(own0.at[f, k], d_recv.at[f, 0, k])
            arrived(own1.at[f, k], d_recv.at[f, 1, k])
        left = jnp.sum(own0[f].astype(F32), axis=0)
        right = jnp.sum(own1[f].astype(F32), axis=0)
        return jnp.concatenate([left, right], axis=1)

    for d in range(1, n):
        send(gains.at[tp], gains.at[tp], gain_send.at[d], gain_recv.at[d], at(z, y, up(tp, d)))
    spread(0, hid)
    send_weights(0, 0)
    send_weights(1, 0)
    gather(0)
    pass_weights(0, 0)
    pass_weights(1, 0)
    for d in range(1, n):
        arrived(gains.at[up(tp, n - d)], gain_recv.at[d])
    take_weights(0, 0)
    gathered(0)
    units = inner_units(0)
    take_weights(1, 0)
    scatter(0, units)
    send_weights(0, 1)
    send_weights(1, 1)
    reduce(0)
    pass_weights(0, 1)
    pass_weights(1, 1)
    first = (hid[...].astype(F32) + 0.5 * reduced(0)).astype(BF16)

    rows_in[tp] = first
    for d in range(1, n):
        send(rows_in.at[tp], rows_in.at[tp], x_send.at[d], x_recv.at[d], at(z, y, up(tp, d)))
    for load in loads[8:]:
        load.wait()
    for d in range(1, n):
        arrived(rows_in.at[up(tp, n - d)], x_recv.at[d])
    squares = jnp.zeros((ROWS, WIDTH), F32)
    for t in range(n):
        values = rows_in[t].astype(F32)
        squares += values * values
    inverse = lax.rsqrt(jnp.sum(squares, axis=1, keepdims=True) / (n * WIDTH) + 1e-06)
    projected = jnp.zeros((ROWS, 4 * HEAD), F32)
    for t in range(n):
        normed = (rows_in[t].astype(F32) * inverse * par[t : t + 1, :]).astype(BF16)
        projected += jnp.dot(
            normed, wmix[t * WIDTH : (t + 1) * WIDTH, :], preferred_element_type=F32
        )
    query = projected[:, 0:HEAD]
    query = query * jax.nn.sigmoid(query)
    floor = par[10:11, 0:HEAD]
    keep = floor + (1.0 - floor) * jax.nn.sigmoid(projected[:, HEAD : 2 * HEAD])
    fresh = (1.0 - floor) * jax.nn.sigmoid(-projected[:, HEAD : 2 * HEAD])
    value = projected[:, 2 * HEAD : 3 * HEAD]
    outgate = projected[:, 3 * HEAD :]
    columns = jnp.concatenate(
        [keep, fresh, query, jnp.zeros((HEAD - 3 * ROWS, HEAD), F32)], axis=0
    ).T
    readout = []
    for b in range(ROWS):
        updated = (
            columns[:, b : b + 1] * state[b]
            + columns[:, ROWS + b : ROWS + b + 1] * value[b : b + 1, :]
        )
        state[b] = updated
        readout.append(
            jnp.sum(columns[:, 2 * ROWS + b : 2 * ROWS + b + 1] * updated, axis=0, keepdims=True)
        )
    readout = jnp.concatenate(readout, axis=0)
    normed = (
        readout
        * lax.rsqrt(jnp.mean(readout * readout, axis=1, keepdims=True) + 1e-05)
        * par[10:11, HEAD : 2 * HEAD]
    )
    gated = (normed * (outgate * jax.nn.sigmoid(outgate))).astype(BF16)
    for t in range(n):
        mix_send[t] = jnp.dot(
            gated, wout[:, t * WIDTH : (t + 1) * WIDTH], preferred_element_type=F32
        ).astype(BF16)
    for d in range(1, n):
        to = up(tp, d)
        send(mix_send.at[to], mix_recv.at[d], m_send.at[d], m_recv.at[d], at(z, y, to))
    store_state = pltpu.make_async_copy(state, state_out_hbm, load_sem.at[14])
    store_state.start()
    mixed = mix_send[tp].astype(F32)
    for d in range(1, n):
        arrived(mix_recv.at[d], m_recv.at[d])
        mixed += mix_recv[d].astype(F32)
    second = (first.astype(F32) + mixed).astype(BF16)
    mid[...] = second

    spread(1, mid)
    gather(1)
    take_weights(0, 1)
    take_weights(1, 1)
    gathered(1)
    scatter(1, inner_units(1))
    reduce(1)
    last[...] = (second.astype(F32) + 0.5 * reduced(1)).astype(BF16)
    store = pltpu.make_async_copy(last, hidden_out_hbm, load_sem.at[15])
    store.start()
    for copy, here in sends:
        if here is None:
            copy.wait_send()
        else:

            @pl.when(jnp.logical_not(here))
            def _():
                copy.wait_send()

    store_state.wait()
    store.wait()


def layer(
    hidden_in,
    first_gain,
    first_gate_proj,
    first_up_proj,
    first_down_proj,
    mix_gain,
    query_weight,
    forget_weight,
    input_weight,
    outgate_weight,
    forget_floor,
    state_in,
    out_gain,
    mix_out_weight,
    second_gain,
    second_gate_proj,
    second_up_proj,
    second_down_proj,
):
    n = lax.axis_size("tp")
    assert lax.axis_size("kv") == n * n
    params = jnp.concatenate(
        [
            jnp.pad(mix_gain.astype(F32).reshape(n, WIDTH), ((0, 8 - n), (0, 0))),
            first_gain.astype(F32)[None],
            second_gain.astype(F32)[None],
            jnp.concatenate([forget_floor, out_gain.astype(F32)])[None],
            jnp.zeros((5, WIDTH), F32),
        ]
    )
    state_shape = (ROWS, HEAD, HEAD)
    dma = pltpu.SemaphoreType.DMA
    vmem = pltpu.VMEM
    any_space = pl.BlockSpec(memory_space=pl.ANY)
    hidden_out, state_out = pl.pallas_call(
        functools.partial(kernel, n),
        out_shape=(
            jax.ShapeDtypeStruct((ROWS, WIDTH), BF16),
            jax.ShapeDtypeStruct(state_shape, F32),
        ),
        in_specs=[any_space] * 14,
        out_specs=(any_space, any_space),
        scratch_shapes=[
            vmem((ROWS, WIDTH), BF16),
            vmem((16, WIDTH), F32),
            vmem((n, 8, WIDTH), F32),
            vmem((2, n, 3, HID, WIDTH), BF16),
            vmem((n * WIDTH, 4 * HEAD), BF16),
            vmem((HEAD, n * WIDTH), BF16),
            vmem(state_shape, F32),
            vmem((2, n, n * ROWS, WIDTH), BF16),
            vmem((2, n, n * ROWS, WIDTH), BF16),
            vmem((2, n, n, ROWS, HALF), BF16),
            vmem((2, n, n, ROWS, HALF), BF16),
            vmem((2, n, ROWS, HALF), BF16),
            vmem((2, n, ROWS, HALF), BF16),
            vmem((2, n, ROWS, HALF), BF16),
            vmem((2, n, ROWS, HALF), BF16),
            vmem((ROWS, WIDTH), BF16),
            vmem((n, ROWS, WIDTH), BF16),
            vmem((n, ROWS, WIDTH), BF16),
            vmem((n, ROWS, WIDTH), BF16),
            vmem((ROWS, WIDTH), BF16),
            dma((16,)),
            dma((n,)),
            dma((n,)),
            dma((2, 2, n)),
            dma((2, 2, n)),
            dma((2, 2, n)),
            dma((2, 2, n)),
            dma((2, 2, n)),
            dma((2, 2, n)),
            dma((2, 2, n)),
            dma((2, 2, n)),
            dma((2, 2, n)),
            dma((2, 2, n)),
            dma((n,)),
            dma((n,)),
            dma((n,)),
            dma((n,)),
        ],
        compiler_params=pltpu.CompilerParams(
            collective_id=0, has_side_effects=True, vmem_limit_bytes=60 * 1024 * 1024
        ),
        name="layer",
    )(
        hidden_in,
        params,
        first_gate_proj.T,
        first_up_proj.T,
        first_down_proj,
        second_gate_proj.T,
        second_up_proj.T,
        second_down_proj,
        query_weight,
        forget_weight,
        input_weight,
        outgate_weight,
        mix_out_weight,
        state_in.reshape(state_shape),
    )
    return hidden_out, state_out.reshape(ROWS, 1, HEAD, HEAD)


def solution(mesh):
    placed = (
        P("kv", "tp"),
        P("tp"),
        P("tp", "kv"),
        P("tp", "kv"),
        P("kv", "tp"),
        P(),
        P(None, "tp"),
        P(None, "tp"),
        P(None, "tp"),
        P(None, "tp"),
        P("tp"),
        P("kv", "tp", None, None),
        P("tp"),
        P("tp", None),
        P("tp"),
        P("tp", "kv"),
        P("tp", "kv"),
        P("kv", "tp"),
    )
    return jax.shard_map(
        layer,
        mesh=mesh,
        in_specs=placed,
        out_specs=(P("kv", "tp"), P("kv", "tp", None, None)),
        check_vma=False,
    )
```

```python
import functools

import jax
import jax.numpy as jnp
from jax import lax
from jax.experimental import pallas as pl
from jax.experimental.pallas import tpu as pltpu
from jax.sharding import PartitionSpec as P

MESH = pl.DeviceIdType.MESH
F32 = jnp.float32
BF16 = jnp.bfloat16
ROWS = 16
WIDTH = 256
HALF = 128
HID = 88
HEAD = 128
PIECES = 4
GATE, UP, DOWN = 0, 1, 2
ROW_DIMS = (((1,), (1,)), ((), ()))


def kernel(
    n,
    hidden_hbm,
    mix_gain_hbm,
    first_gain_hbm,
    second_gain_hbm,
    floor_hbm,
    out_gain_hbm,
    gate1_hbm,
    up1_hbm,
    down1_hbm,
    gate2_hbm,
    up2_hbm,
    down2_hbm,
    query_hbm,
    forget_hbm,
    input_hbm,
    outgate_hbm,
    mixout_hbm,
    state_hbm,
    hidden_out_hbm,
    state_out_hbm,
    hid,
    mix_gain,
    own_gains,
    floor_in,
    out_gain,
    gains,
    weights,
    wmix,
    wout,
    state,
    act,
    part,
    red0,
    red1,
    sum0,
    sum1,
    own0,
    own1,
    mid,
    rows_in,
    mix_send,
    mix_recv,
    last,
    load_sem,
    gain_send,
    gain_recv,
    w_send,
    w_recv,
    p_send,
    p_recv,
    a_send,
    a_recv,
    b_send,
    b_recv,
    c_send,
    c_recv,
    d_send,
    d_recv,
    x_send,
    x_recv,
    m_send,
    m_recv,
):
    kv = lax.axis_index("kv")
    tp = lax.axis_index("tp")
    z, y = lax.div(kv, n), lax.rem(kv, n)
    group = lax.rem(z + y, n)
    src_y = lax.rem(tp - z + n, n)
    src_z = lax.rem(tp - y + n, n)
    home = tp == group
    pair = tp + 1 - 2 * lax.rem(tp, 2)
    far_first = sorted(range(1, n), key=lambda d: -min(d, n - d))

    def at(zz, yy, tt):
        return {"kv": zz * n + yy, "tp": tt}

    def up(index, d):
        return lax.rem(index + d, n)

    def rows_of(zz):
        return pl.ds(pl.multiple_of(zz * ROWS, ROWS), ROWS)

    early = [
        (hidden_hbm, hid),
        (first_gain_hbm, own_gains.at[0]),
        (second_gain_hbm, own_gains.at[1]),
        (gate1_hbm, weights.at[0, tp, GATE]),
        (up1_hbm, weights.at[0, tp, UP]),
        (down1_hbm, weights.at[0, tp, DOWN]),
    ]
    later = [
        (gate2_hbm, weights.at[1, tp, GATE]),
        (up2_hbm, weights.at[1, tp, UP]),
        (down2_hbm, weights.at[1, tp, DOWN]),
        (mix_gain_hbm, mix_gain),
        (floor_hbm, floor_in),
        (out_gain_hbm, out_gain),
        (query_hbm, wmix.at[:, 0:HEAD]),
        (forget_hbm, wmix.at[:, HEAD : 2 * HEAD]),
        (input_hbm, wmix.at[:, 2 * HEAD : 3 * HEAD]),
        (outgate_hbm, wmix.at[:, 3 * HEAD :]),
        (mixout_hbm, wout),
        (state_hbm, state),
    ]
    loads = [
        pltpu.make_async_copy(src, dst, load_sem.at[i])
        for i, (src, dst) in enumerate(early + later)
    ]
    for load in loads:
        load.start()

    barrier = pltpu.get_barrier_semaphore()

    def greet(device):
        pl.semaphore_signal(barrier, inc=1, device_id=device, device_id_type=MESH)

    for d in range(1, n):
        greet(at(z, y, up(tp, d)))
        greet(at(up(z, d), y, tp))
        greet(at(z, up(y, d), tp))
        greet(at(z, up(y, d), group))
        greet(at(up(z, d), y, group))

    @pl.when(jnp.logical_not(home))
    def _():
        for d in range(n):
            greet(at(z, src_y, up(tp, d)))
            greet(at(src_z, y, up(tp, d)))

    with jax.named_scope("load"):
        for load in loads[: len(early)]:
            load.wait()
        for f in range(2):
            gains[tp, 2 * f : 2 * f + 2] = own_gains[f].astype(F32)

    with jax.named_scope("meet"):
        pl.semaphore_wait(barrier, 5 * (n - 1) + jnp.where(home, 0, 2 * n))

    def send(src, dst, send_sem, recv_sem, device):
        pltpu.make_async_remote_copy(
            src_ref=src,
            dst_ref=dst,
            send_sem=send_sem,
            recv_sem=recv_sem,
            device_id=device,
            device_id_type=MESH,
        ).start()

    def send_or_keep(here, src, dst, send_sem, recv_sem, device):
        @pl.when(here)
        def _():
            pltpu.make_async_copy(src, dst, recv_sem).start()

        @pl.when(jnp.logical_not(here))
        def _():
            send(src, dst, send_sem, recv_sem, device)

    def through(ref, sem):
        pltpu.make_async_copy(ref, ref, sem).wait()

    def weights_of(kind, f, slot):
        return weights.at[f, slot, GATE:DOWN] if kind == 0 else weights.at[f, slot, DOWN]

    def some_weights(kind, f, count):
        return weights.at[f, 0:count, GATE:DOWN] if kind == 0 else weights.at[f, 0:count, DOWN]

    def send_weights(kind, f):
        block = weights_of(kind, f, tp)
        for k in range(1, n // 2):
            send(block, block, w_send.at[kind, f], w_recv.at[kind, f], at(z, y, up(tp, 2 * k)))
        send(block, block, p_send.at[kind, f], p_recv.at[kind, f], at(z, y, pair))

    def pass_weights(kind, f):
        if n > 2:
            through(some_weights(kind, f, n // 2 - 1), w_recv.at[kind, f])
        for k in range(1, n // 2):
            block = weights_of(kind, f, up(tp, 2 * k))
            send(block, block, p_send.at[kind, f], p_recv.at[kind, f], at(z, y, pair))

    def take_weights(kind, f):
        through(some_weights(kind, f, n // 2), p_recv.at[kind, f])

    def weights_sent(kind, f):
        if n > 2:
            through(some_weights(kind, f, n // 2 - 1), w_send.at[kind, f])
        through(some_weights(kind, f, n // 2), p_send.at[kind, f])

    def spread(f, block):
        mine = act.at[f, tp, rows_of(z)]
        for d in [0] + far_first:
            for half, lanes, device in (
                (0, slice(0, HALF), at(z, up(y, d), group)),
                (1, slice(HALF, WIDTH), at(up(z, d), y, group)),
            ):
                args = (
                    block.at[:, lanes],
                    mine.at[:, lanes],
                    a_send.at[f, half],
                    a_recv.at[f, half],
                    device,
                )
                if d == 0:
                    send_or_keep(home, *args)
                else:
                    send(*args)

    def gather(f):
        for half, lanes, row in ((0, slice(0, HALF), z), (1, slice(HALF, WIDTH), src_z)):
            region = act.at[f, :, rows_of(row), lanes]
            through(region, a_recv.at[f, half])
            for d in far_first:
                device = at(up(z, d), y, tp) if half == 0 else at(z, up(y, d), tp)
                send(region, region, b_send.at[f, half], b_recv.at[f, half], device)

    def gathered(f):
        through(act.at[f, 0 : n - 1, :, 0:HALF], b_recv.at[f, 0])
        through(act.at[f, 0 : n - 1, :, HALF:WIDTH], b_recv.at[f, 1])

    def inner_units(f):
        gate = jnp.zeros((n * ROWS, HID), F32)
        up_total = jnp.zeros((n * ROWS, HID), F32)
        squares = jnp.zeros((n * ROWS, HALF), F32)
        for t in range(n):
            values = act[f, t].astype(F32)
            squares += values[:, 0:HALF] * values[:, 0:HALF]
            squares += values[:, HALF:WIDTH] * values[:, HALF:WIDTH]
            gain = jnp.concatenate(
                [gains[t, 2 * f : 2 * f + 1, :], gains[t, 2 * f + 1 : 2 * f + 2, :]], axis=1
            )
            scaled = (values * gain).astype(BF16)
            gate += lax.dot_general(scaled, weights[f, t, GATE], ROW_DIMS, preferred_element_type=F32)
            up_total += lax.dot_general(scaled, weights[f, t, UP], ROW_DIMS, preferred_element_type=F32)
        inverse = lax.rsqrt(jnp.sum(squares, axis=1, keepdims=True) / (n * WIDTH) + 1e-06)
        gate = gate * inverse
        return (gate * jax.nn.sigmoid(gate) * (up_total * inverse)).astype(BF16)

    def scatter(f, units):
        for t in range(n):
            part[f, t] = jnp.dot(
                units, weights[f, t, DOWN], preferred_element_type=F32
            ).astype(BF16)
        for d in far_first:
            to_z, to_y = up(z, d), up(y, d)
            send(
                part.at[f, :, rows_of(to_z), 0:HALF],
                red0.at[f, d],
                c_send.at[f, 0],
                c_recv.at[f, 0],
                at(to_z, y, tp),
            )
            send(
                part.at[f, :, rows_of(lax.rem(tp - to_y + n, n)), HALF:WIDTH],
                red1.at[f, d],
                c_send.at[f, 1],
                c_recv.at[f, 1],
                at(z, to_y, tp),
            )

    def reduce(f):
        for half, red, summed, lanes, row in (
            (0, red0, sum0, slice(0, HALF), z),
            (1, red1, sum1, slice(HALF, WIDTH), src_z),
        ):
            total = part[f, :, rows_of(row), lanes].astype(F32)
            through(red.at[f, 1:n], c_recv.at[f, half])
            for d in range(1, n):
                total += red[f, d].astype(F32)
            summed[f] = total.astype(BF16)
            for e in [0] + far_first:
                tt = up(tp, e)
                if half == 0:
                    args = (sum0.at[f, tt], own0.at[f, y], d_send.at[f, 0], d_recv.at[f, 0])
                    device = at(z, src_y, tt)
                else:
                    args = (sum1.at[f, tt], own1.at[f, z], d_send.at[f, 1], d_recv.at[f, 1])
                    device = at(src_z, y, tt)
                if e == 0:
                    send_or_keep(home, *args, device)
                else:
                    send(*args, device)

    def reduced(f):
        through(own0.at[f], d_recv.at[f, 0])
        through(own1.at[f], d_recv.at[f, 1])
        left = jnp.sum(own0[f].astype(F32), axis=0)
        right = jnp.sum(own1[f].astype(F32), axis=0)
        return jnp.concatenate([left, right], axis=1)

    with jax.named_scope("start"):
        for d in range(1, n):
            send(
                gains.at[tp], gains.at[tp], gain_send, gain_recv, at(z, y, up(tp, d))
            )
        spread(0, hid)
        send_weights(0, 0)
        send_weights(1, 0)
    with jax.named_scope("gather1"):
        gather(0)
    with jax.named_scope("pass1"):
        pass_weights(0, 0)
        pass_weights(1, 0)
        through(gains.at[1:n], gain_recv)
        take_weights(0, 0)
    with jax.named_scope("gathered1"):
        gathered(0)
    with jax.named_scope("inner1"):
        units = inner_units(0)
    with jax.named_scope("scatter1"):
        take_weights(1, 0)
        scatter(0, units)
        for load in loads[len(early) : len(early) + 3]:
            load.wait()
        send_weights(0, 1)
        send_weights(1, 1)
    with jax.named_scope("reduce1"):
        reduce(0)
    with jax.named_scope("pass2"):
        pass_weights(0, 1)
        pass_weights(1, 1)
    with jax.named_scope("reduced1"):
        first = (hid[...].astype(F32) + 0.5 * reduced(0)).astype(BF16)
        rows_in[tp] = first

    for d in range(1, n):
        send(rows_in.at[tp], rows_in.at[tp], x_send, x_recv, at(z, y, up(tp, d)))
    with jax.named_scope("rows"):
        for load in loads[len(early) + 3 :]:
            load.wait()
        through(rows_in.at[1:n], x_recv)
    squares = jnp.zeros((ROWS, WIDTH), F32)
    for t in range(n):
        values = rows_in[t].astype(F32)
        squares += values * values
    inverse = lax.rsqrt(jnp.sum(squares, axis=1, keepdims=True) / (n * WIDTH) + 1e-06)
    projected = jnp.zeros((ROWS, 4 * HEAD), F32)
    mix_gains = mix_gain[...].astype(F32)
    for t in range(n):
        gain = jnp.concatenate(
            [mix_gains[2 * t : 2 * t + 1, :], mix_gains[2 * t + 1 : 2 * t + 2, :]], axis=1
        )
        normed = (rows_in[t].astype(F32) * inverse * gain).astype(BF16)
        projected += jnp.dot(
            normed, wmix[t * WIDTH : (t + 1) * WIDTH, :], preferred_element_type=F32
        )
    query = projected[:, 0:HEAD]
    query = query * jax.nn.sigmoid(query)
    floor = floor_in[...]
    keep = floor + (1.0 - floor) * jax.nn.sigmoid(projected[:, HEAD : 2 * HEAD])
    fresh = (1.0 - floor) * jax.nn.sigmoid(-projected[:, HEAD : 2 * HEAD])
    value = projected[:, 2 * HEAD : 3 * HEAD]
    outgate = projected[:, 3 * HEAD :]
    columns = jnp.concatenate(
        [keep, fresh, query, jnp.zeros((HEAD - 3 * ROWS, HEAD), F32)], axis=0
    ).T
    readout = []
    for b in range(ROWS):
        updated = (
            columns[:, b : b + 1] * state[b]
            + columns[:, ROWS + b : ROWS + b + 1] * value[b : b + 1, :]
        )
        state[b] = updated
        readout.append(
            jnp.sum(columns[:, 2 * ROWS + b : 2 * ROWS + b + 1] * updated, axis=0, keepdims=True)
        )
    readout = jnp.concatenate(readout, axis=0)
    normed = (
        readout
        * lax.rsqrt(jnp.mean(readout * readout, axis=1, keepdims=True) + 1e-05)
        * out_gain[...].astype(F32)
    )
    gated = (normed * (outgate * jax.nn.sigmoid(outgate))).astype(BF16)
    for t in range(n):
        mix_send[t] = jnp.dot(
            gated, wout[:, t * WIDTH : (t + 1) * WIDTH], preferred_element_type=F32
        ).astype(BF16)
    for d in range(1, n):
        to = up(tp, d)
        send(mix_send.at[to], mix_recv.at[d], m_send, m_recv, at(z, y, to))
    store_state = pltpu.make_async_copy(state, state_out_hbm, load_sem.at[18])
    store_state.start()
    with jax.named_scope("mixed"):
        mixed = mix_send[tp].astype(F32)
        through(mix_recv.at[1:n], m_recv)
        for d in range(1, n):
            mixed += mix_recv[d].astype(F32)
        second = (first.astype(F32) + mixed).astype(BF16)
        mid[...] = second

    with jax.named_scope("gather2"):
        spread(1, mid)
        gather(1)
    with jax.named_scope("take2"):
        take_weights(0, 1)
        take_weights(1, 1)
    with jax.named_scope("gathered2"):
        gathered(1)
    with jax.named_scope("inner2"):
        units = inner_units(1)
    with jax.named_scope("scatter2"):
        scatter(1, units)
    with jax.named_scope("reduce2"):
        reduce(1)
    with jax.named_scope("reduced2"):
        last[...] = (second.astype(F32) + 0.5 * reduced(1)).astype(BF16)
    store = pltpu.make_async_copy(last, hidden_out_hbm, load_sem.at[19])
    store.start()
    with jax.named_scope("sent"):
        through(gains.at[1:n], gain_send)
        through(rows_in.at[1:n], x_send)
        through(mix_recv.at[1:n], m_send)
        for f in range(2):
            for kind in range(2):
                weights_sent(kind, f)
            for half, red in ((0, red0), (1, red1)):
                through(red.at[f, 1:n], b_send.at[f, half])
                through(red.at[f, 1:n], c_send.at[f, half])
                through(sum0.at[f, 1:n], a_send.at[f, half])
                through(sum0.at[f, 1:n], d_send.at[f, half])

        @pl.when(jnp.logical_not(home))
        def _():
            for f in range(2):
                for half in range(2):
                    through(sum0.at[f, 0], a_send.at[f, half])
                    through(sum0.at[f, 0], d_send.at[f, half])

    store_state.wait()
    store.wait()


def hand_over(hidden_hbm, state_hbm, hidden_out_hbm, state_out_hbm, hid, state, in_sem, out_sem):
    rows = ROWS // PIECES
    parts = [(hidden_hbm, hid, hidden_out_hbm)]
    for i in range(PIECES):
        part = pl.ds(i * rows, rows)
        parts.append((state_hbm.at[part], state.at[part], state_out_hbm.at[part]))
    ins = [pltpu.make_async_copy(a, b, in_sem.at[i]) for i, (a, b, _) in enumerate(parts)]
    outs = [pltpu.make_async_copy(b, c, out_sem.at[i]) for i, (_, b, c) in enumerate(parts)]
    for copy in ins:
        copy.start()
    for copy, onward in zip(ins, outs):
        copy.wait()
        onward.start()
    for onward in outs:
        onward.wait()


def layer(
    hidden_in,
    first_gain,
    first_gate_proj,
    first_up_proj,
    first_down_proj,
    mix_gain,
    query_weight,
    forget_weight,
    input_weight,
    outgate_weight,
    forget_floor,
    state_in,
    out_gain,
    mix_out_weight,
    second_gain,
    second_gate_proj,
    second_up_proj,
    second_down_proj,
):
    n = lax.axis_size("tp")
    assert lax.axis_size("kv") == n * n
    state_shape = (ROWS, HEAD, HEAD)
    dma = pltpu.SemaphoreType.DMA
    vmem = pltpu.VMEM
    any_space = pl.BlockSpec(memory_space=pl.ANY)
    hidden_out, state_out = pl.pallas_call(
        functools.partial(kernel, n),
        out_shape=(
            jax.ShapeDtypeStruct((ROWS, WIDTH), BF16),
            jax.ShapeDtypeStruct(state_shape, F32),
        ),
        in_specs=[any_space] * 18,
        out_specs=(any_space, any_space),
        scratch_shapes=[
            vmem((ROWS, WIDTH), BF16),
            vmem((2 * n, HALF), BF16),
            vmem((2, 2, HALF), BF16),
            vmem((1, HEAD), F32),
            vmem((1, HEAD), BF16),
            vmem((n, 8, HALF), F32),
            vmem((2, n, 3, HID, WIDTH), BF16),
            vmem((n * WIDTH, 4 * HEAD), BF16),
            vmem((HEAD, n * WIDTH), BF16),
            vmem(state_shape, F32),
            vmem((2, n, n * ROWS, WIDTH), BF16),
            vmem((2, n, n * ROWS, WIDTH), BF16),
            vmem((2, n, n, ROWS, HALF), BF16),
            vmem((2, n, n, ROWS, HALF), BF16),
            vmem((2, n, ROWS, HALF), BF16),
            vmem((2, n, ROWS, HALF), BF16),
            vmem((2, n, ROWS, HALF), BF16),
            vmem((2, n, ROWS, HALF), BF16),
            vmem((ROWS, WIDTH), BF16),
            vmem((n, ROWS, WIDTH), BF16),
            vmem((n, ROWS, WIDTH), BF16),
            vmem((n, ROWS, WIDTH), BF16),
            vmem((ROWS, WIDTH), BF16),
            dma((20,)),
            dma,
            dma,
            dma((2, 2)),
            dma((2, 2)),
            dma((2, 2)),
            dma((2, 2)),
            dma((2, 2)),
            dma((2, 2)),
            dma((2, 2)),
            dma((2, 2)),
            dma((2, 2)),
            dma((2, 2)),
            dma((2, 2)),
            dma((2, 2)),
            dma,
            dma,
            dma,
            dma,
        ],
        compiler_params=pltpu.CompilerParams(
            collective_id=0, has_side_effects=True, vmem_limit_bytes=60 * 1024 * 1024
        ),
        name="layer",
    )(
        hidden_in,
        mix_gain.reshape(2 * n, HALF),
        first_gain.reshape(2, HALF),
        second_gain.reshape(2, HALF),
        forget_floor.reshape(1, HEAD),
        out_gain.reshape(1, HEAD),
        first_gate_proj.T,
        first_up_proj.T,
        first_down_proj,
        second_gate_proj.T,
        second_up_proj.T,
        second_down_proj,
        query_weight,
        forget_weight,
        input_weight,
        outgate_weight,
        mix_out_weight,
        state_in.reshape(state_shape),
    )
    hidden_out, state_out = pl.pallas_call(
        hand_over,
        out_shape=(
            jax.ShapeDtypeStruct((ROWS, WIDTH), BF16),
            jax.ShapeDtypeStruct(state_shape, F32),
        ),
        in_specs=[any_space] * 2,
        out_specs=(any_space, any_space),
        scratch_shapes=[
            vmem((ROWS, WIDTH), BF16),
            vmem(state_shape, F32),
            dma((PIECES + 1,)),
            dma((PIECES + 1,)),
        ],
        compiler_params=pltpu.CompilerParams(vmem_limit_bytes=60 * 1024 * 1024),
        name="hand_over",
    )(hidden_out, state_out)
    return hidden_out, state_out.reshape(ROWS, 1, HEAD, HEAD)


def solution(mesh):
    placed = (
        P("kv", "tp"),
        P("tp"),
        P("tp", "kv"),
        P("tp", "kv"),
        P("kv", "tp"),
        P(),
        P(None, "tp"),
        P(None, "tp"),
        P(None, "tp"),
        P(None, "tp"),
        P("tp"),
        P("kv", "tp", None, None),
        P("tp"),
        P("tp", None),
        P("tp"),
        P("tp", "kv"),
        P("tp", "kv"),
        P("kv", "tp"),
    )
    return jax.shard_map(
        layer,
        mesh=mesh,
        in_specs=placed,
        out_specs=(P("kv", "tp"), P("kv", "tp", None, None)),
        check_vma=False,
    )
```
